32 devices in a mesh: sp: 8 (over z, y), tp: 4 (over x, core).
Axes of the slice: x: 2, y: 2, z: 4, core: 2. Of those that a mesh axis runs over, the one named last changes fastest.
Arguments:
- resid: bfloat16 [6144, 4096], P(('sp', 'tp')), may hold values from -80 to 80
- pool_in: bfloat16 [6144, 1024], P('sp', 'tp'), may hold values from -6 to 6
- pool_weight: bfloat16 [4, 256, 256], P('tp'), may hold values from -0.375 to 0.375
- pool_scale: float32 [1024], P('tp'), may hold values from 0.1 to 1.9
- out_weight: bfloat16 [1024, 4096], P('tp'), may hold values from -0.1875 to 0.1875
- norm_gain: float32 [4096], replicated, may hold values from 0.1 to 1.9
- route_ids: int32 [6144, 4], P(('sp', 'tp')), may hold values from 0 to 31, all different within a row; in each aligned block of 192 rows (0 to 191, 192 to 383, ...) at most 36 rows name the same one
- route_weight: float32 [6144, 4], P(('sp', 'tp')), may hold values from 0.1 to 1
- expert_gate: bfloat16 [32, 4096, 384], P('sp'), may hold values from -0.09375 to 0.09375
- expert_up: bfloat16 [32, 4096, 384], P('sp'), may hold values from -0.09375 to 0.09375
- expert_down: bfloat16 [32, 384, 4096], P('sp'), may hold values from -0.3125 to 0.3125
- shared_gate: bfloat16 [4096, 384], replicated, may hold values from -0.09375 to 0.09375
- shared_up: bfloat16 [4096, 384], replicated, may hold values from -0.09375 to 0.09375
- shared_down: bfloat16 [384, 4096], replicated, may hold values from -0.3125 to 0.3125
Outputs:
- layer_out: bfloat16 [6144, 4096], P(('sp', 'tp'))
The draws below stay inside these ranges and needn't reach their ends.
Inputs may be any that keep to these rules, and one draw needn't show every extreme that they name: `route_ids`: each row names 4 different experts. Among the rows of one device no expert is named more than 36 times, and that count is reached.
All inputs are finite; a program needn't handle non-finite values.
Results may differ from the reference program's by a relative error of at most 0.012.
Values may be sent and summed in bfloat16 or wider, within the bound.
No kernel may reach another device: no remote copies, remote signals or barrier semaphores. Data moves between devices by JAX's collectives and lax.ppermute only.
A program may use at most 192 MiB of HBM per device.

```python
import math
import jax
import jax.numpy as jnp
import numpy as np
from jax import lax

D = 4096
POOL_WIDTH = 1024
POOL_GROUP = 256
FE = 384
FS = 384
EXPERTS = 32
TOP_K = 4
TOK_DEV = 768
TOKENS = 6144
CAP = 36
N_SP = 8
N_TP = 4


def draw_resid(key, part):
    base = jnp.clip(jax.random.normal(jax.random.fold_in(key, 11), (TOKENS, D), jnp.float32), -6.0, 6.0)
    column_scale = 0.3 * 10.0 ** jax.random.uniform(jax.random.fold_in(key, 12), (D,), jnp.float32)
    return (base * column_scale[None, :]).astype(jnp.bfloat16)


def steps_of(stream_key, shape, cuts, least, high):
    gain, own = 1.0, jax.random.fold_in(stream_key, 6)
    for position, blocks in cuts:
        steps = jnp.exp(jax.random.uniform(jax.random.fold_in(own, position), (blocks,), jnp.float32, least / len(cuts), high / len(cuts)))
        gain = gain * jnp.repeat(steps, shape[position] // blocks).reshape([-1 if axis == position else 1 for axis in range(len(shape))])
    return gain


def assign_block(key, own, number, rows, amount, top, most, lean):
    ranking = jax.random.permutation(key, amount)
    crowded, ordinary = portions_of(amount, rows * top, most, lean, True), portions_of(amount, rows * top, most, lean, False)
    places = jnp.arange(amount)

    def named(sizes, turn):
        used = int((sizes > 0).sum())
        fixed = max(1, used // 4)
        moved = fixed + (places - fixed + turn * (used - fixed)) % max(1, amount - fixed)
        return jnp.zeros((amount,), jnp.int32).at[ranking[jnp.where(places < fixed, places, moved)]].set(jnp.asarray(sizes, jnp.int32))

    sizes = jnp.where(number % 4 == 0, named(crowded, number // 4), named(ordinary, number - number // 4 - 1))
    mixed = jax.random.permutation(jax.random.fold_in(own, 3), amount)
    source_of, receiver = mixed[0:amount // 2 * 2:2], mixed[1:amount // 2 * 2:2]
    margin = jnp.minimum(sizes[source_of] - 1, most - sizes[receiver]) // 2
    margin = jnp.where((source_of == ranking[0]) | (receiver == ranking[0]) | (sizes[receiver] == 0), 0, jnp.maximum(margin, 0))
    moved = jax.random.randint(jax.random.fold_in(own, 4), (amount // 2,), 0, 1 << 20) % (margin + 1)
    sizes = sizes.at[source_of].add(-moved).at[receiver].add(moved)
    labels = jnp.searchsorted(jnp.cumsum(sizes), jnp.arange(rows * top), side="right").astype(jnp.int32)
    grid = labels.reshape(top, rows).T
    grid = grid[jax.random.permutation(jax.random.fold_in(own, 1), rows)]
    turn = jax.random.randint(jax.random.fold_in(own, 2), (rows, 1), 0, top)
    return jnp.take_along_axis(grid, (jnp.arange(top)[None, :] + turn) % top, axis=1)


def portions_of(number_of, total, bound, lean, full):
    loads = [(1 << 20) // math.isqrt(standing ** lean) + 1 for standing in range(1, number_of + 1)]
    largest = bound if full else min(bound, max(-(-total // number_of), total * loads[0] // sum(loads)))
    least = 1 if total - largest >= number_of - 1 else 0
    given, spare = [largest] + [least] * (number_of - 1), total - largest - least * (number_of - 1)
    while spare > 0:
        candidates = [i for i in range(1, number_of) if given[i] < largest] or [i for i in range(1, number_of) if given[i] < bound]
        whole, budget = sum([loads[i] for i in candidates]), spare
        for i in candidates:
            extra = min(bound - given[i], max(1, budget * loads[i] // whole), spare)
            given[i] = given[i] + extra
            spare = spare - extra
    return np.array(given)


def noise(stream_key, shape, scale, bound, shards=(), held_as=jnp.bfloat16):
    loudness = steps_of(stream_key, shape, shards, -0.22, 0.18) if shards else 1.0
    values = jax.random.normal(stream_key, shape, jnp.float32) * scale * loudness
    return jnp.minimum(jnp.maximum(values, -bound), bound).astype(held_as)


def setup_inputs(seed: int = 0) -> dict:
    seeds = jax.random.split(jax.random.key(seed), 15)
    resid = draw_resid(jax.random.fold_in(seeds[14], 71), 0)
    pool_in = noise(seeds[1], (TOKENS, POOL_WIDTH), 1.0, 6.0, ((0, 8), (1, 4)))
    pool_weight = noise(seeds[2], (4, POOL_GROUP, POOL_GROUP), POOL_GROUP ** -0.5, 0.375, ((0, 4),))
    pool_scale = jnp.clip(1.0 + 0.18 * jax.random.normal(seeds[3], (POOL_WIDTH,), jnp.float32), 0.1, 1.9)
    out_weight = noise(seeds[4], (POOL_WIDTH, D), POOL_WIDTH ** -0.5, 0.1875, ((0, 4),))
    norm_gain = jnp.clip(1.0 + 0.18 * jax.random.normal(seeds[5], (D,), jnp.float32), 0.1, 1.9)
    route_ids_keys = jax.random.split(jax.random.fold_in(seeds[6], 1), TOKENS // (TOK_DEV // N_TP))
    route_ids_turns = jax.random.permutation(jax.random.fold_in(seeds[6], 3), TOKENS // (TOK_DEV // N_TP))
    route_ids = jax.vmap(lambda own, number: assign_block(jax.random.fold_in(seeds[6], 2), own, number, TOK_DEV // N_TP, EXPERTS, TOP_K, CAP, 1))(route_ids_keys, route_ids_turns).reshape((TOKENS, TOP_K))
    route_weight = jnp.clip(jnp.exp(math.log(1.0) - 2.3025851 * jax.random.uniform(seeds[7], (TOKENS, TOP_K), jnp.float32) ** steps_of(seeds[7], (TOKENS, TOP_K), ((0, 32),), -0.2, 0.2)), 0.1, 1.0)
    expert_gate = noise(seeds[8], (EXPERTS, D, FE), D ** -0.5, 0.09375, ((0, 8),))
    expert_up = noise(seeds[9], (EXPERTS, D, FE), D ** -0.5, 0.09375, ((0, 8),))
    expert_down = noise(seeds[10], (EXPERTS, FE, D), FE ** -0.5, 0.3125, ((0, 8),))
    shared_gate = noise(seeds[11], (D, FS), D ** -0.5, 0.09375)
    shared_up = noise(seeds[12], (D, FS), D ** -0.5, 0.09375)
    shared_down = noise(seeds[13], (FS, D), FS ** -0.5, 0.3125)
    return {"resid": resid, "pool_in": pool_in, "pool_weight": pool_weight, "pool_scale": pool_scale, "out_weight": out_weight, "norm_gain": norm_gain, "route_ids": route_ids, "route_weight": route_weight, "expert_gate": expert_gate, "expert_up": expert_up, "expert_down": expert_down, "shared_gate": shared_gate, "shared_up": shared_up, "shared_down": shared_down}


def pool_mix(pool_in, pool_weight, pool_scale):
    whole_len = pool_in.shape[0]
    group_width = pool_weight.shape[1]
    padded = jnp.pad(pool_in.astype(jnp.float32), ((8, 8), (0, 0)))
    positions = jnp.arange(whole_len, dtype=jnp.int32)
    outputs = []
    for group_num in range(4):
        half_span = 2 ** group_num
        columns = padded[:, group_num * group_width:(group_num + 1) * group_width]
        running = jnp.zeros((whole_len, group_width), jnp.float32)
        for row_shift in range(-half_span, half_span):
            running = running + columns[8 + row_shift:8 + row_shift + whole_len]
        upper_end = jnp.minimum(positions + half_span, whole_len)
        lower_end = jnp.maximum(positions - half_span, 0)
        row_count = (upper_end - lower_end).astype(jnp.float32)
        center = columns[8:8 + whole_len]
        spread = (running / row_count[:, None] - center).astype(jnp.bfloat16)
        outputs.append(jnp.dot(spread, pool_weight[group_num], preferred_element_type=jnp.float32))
    mixed_rows = jnp.concatenate(outputs, axis=1)
    return (mixed_rows * pool_scale[None, :]).astype(jnp.bfloat16)

def reference(resid, pool_in, pool_weight, pool_scale, out_weight, norm_gain, route_ids, route_weight, expert_gate, expert_up, expert_down, shared_gate, shared_up, shared_down):
    pooled = pool_mix(pool_in, pool_weight, pool_scale)
    middle = (resid.astype(jnp.float32) + jnp.dot(pooled, out_weight, preferred_element_type=jnp.float32)).astype(jnp.bfloat16)
    middle_float = middle.astype(jnp.float32)
    square_mean = lax.optimization_barrier(jnp.mean(middle_float * middle_float, axis=1, keepdims=True))
    normed = (middle_float * lax.rsqrt(square_mean + 1e-06) * norm_gain[None, :]).astype(jnp.bfloat16)
    shared_hidden = (jax.nn.silu(jnp.dot(normed, shared_gate, preferred_element_type=jnp.float32)) * jnp.dot(normed, shared_up, preferred_element_type=jnp.float32)).astype(jnp.bfloat16)
    shared_out = jnp.dot(shared_hidden, shared_down, preferred_element_type=jnp.float32)
    tokens_all = normed.shape[0]
    top_count = route_ids.shape[1]
    flat_ids = route_ids.reshape(-1).astype(jnp.int32)
    onehot = (flat_ids[:, None] == jnp.arange(EXPERTS, dtype=jnp.int32)[None, :]).astype(jnp.int32)
    rank_in_expert = lax.optimization_barrier(jnp.sum(jnp.cumsum(onehot, axis=0) * onehot, axis=1)) - 1
    slot_width = N_SP * N_TP * CAP
    sentinel = tokens_all * top_count
    slot_table = jnp.full((EXPERTS, slot_width), sentinel, jnp.int32).at[flat_ids, rank_in_expert].set(jnp.arange(sentinel, dtype=jnp.int32))
    extended = jnp.concatenate([normed, jnp.zeros((1, normed.shape[1]), jnp.bfloat16)], axis=0)
    weight_ext = jnp.concatenate([route_weight.reshape(-1), jnp.zeros((1,), jnp.float32)], axis=0)

    def expert_step(totals, stacked):
        gate_w, up_w, down_w, entries = stacked
        token_rows = entries // top_count
        gathered = jnp.take(extended, token_rows, axis=0)
        hidden = (jax.nn.silu(jnp.dot(gathered, gate_w, preferred_element_type=jnp.float32)) * jnp.dot(gathered, up_w, preferred_element_type=jnp.float32)).astype(jnp.bfloat16)
        produced = jnp.dot(hidden, down_w, preferred_element_type=jnp.float32).astype(jnp.bfloat16)
        weights = jnp.take(weight_ext, entries)
        return (totals.at[token_rows].add(produced.astype(jnp.float32) * weights[:, None]), None)
    start_totals = jnp.zeros((tokens_all + 1, normed.shape[1]), jnp.float32)
    routed, _ = lax.scan(expert_step, start_totals, (expert_gate, expert_up, expert_down, slot_table))
    return (middle_float + shared_out + routed[:tokens_all]).astype(jnp.bfloat16)
```

```python
import functools

import jax
import jax.numpy as jnp
from jax import lax
from jax.experimental import pallas as pl
from jax.experimental.pallas import tpu as pltpu
from jax.sharding import PartitionSpec as P

reach_rows = 8
norm_eps = 1e-06
outer = 4


f32 = jnp.float32
bf16 = jnp.bfloat16


def with_halo(cells, axis, width):
    count = lax.axis_size(axis)
    ends = count - 1
    head = cells[:width]
    tail = cells[cells.shape[0] - width :]
    return jnp.concatenate(
        [
            lax.ppermute(tail, axis, [(i, i + 1) for i in range(ends)]),
            cells,
            lax.ppermute(head, axis, [(i + 1, i) for i in range(ends)]),
        ],
        axis=0,
    )


def window_means(padded, length, offset, whole_len):
    positions = offset + lax.iota(jnp.int32, length)
    running = jnp.zeros((length,) + padded.shape[1:], f32)
    averages = []
    covered = 0
    for section_num in range(4):
        half_span = 2**section_num
        for row_shift in list(range(-half_span, -covered)) + list(range(covered, half_span)):
            running = running + padded[reach_rows + row_shift : reach_rows + row_shift + length]
        covered = half_span
        upper_end = jnp.minimum(positions + half_span, whole_len)
        lower_end = jnp.maximum(positions - half_span, 0)
        row_count = (upper_end - lower_end).astype(f32)
        averages.append(running / row_count[:, None, None])
    return averages


def pool_mix(pool_in, pool_weight, pool_scale):
    tok_local = pool_in.shape[0]
    local_groups, group_width = pool_weight.shape[:2]
    padded = with_halo(pool_in, "sp", reach_rows).astype(f32)
    padded = padded.reshape(tok_local + 2 * reach_rows, local_groups, group_width)
    averages = window_means(
        padded, tok_local, lax.axis_index("sp") * tok_local, tok_local * lax.axis_size("sp")
    )
    center = padded[reach_rows : reach_rows + tok_local]
    group_ids = lax.axis_index("tp") * local_groups + lax.iota(jnp.int32, local_groups)
    chosen = averages[0]
    for section_num in range(1, 4):
        chosen = jnp.where((group_ids == section_num)[None, :, None], averages[section_num], chosen)
    spread = (chosen - center).astype(bf16)
    mixed_rows = jnp.einsum("tgc,gce->tge", spread, pool_weight, preferred_element_type=f32)
    return (mixed_rows.reshape(tok_local, -1) * pool_scale[None, :]).astype(bf16)


def out_norm_kernel(count, *refs):
    pieces, weights = refs[:count], refs[count : 2 * count]
    resid, gain, middle, normed = refs[2 * count :]
    rows, width = resid.shape
    step = 1024
    total = jnp.zeros((rows, 1), f32)
    for lo in range(0, width, step):
        acc = resid[:, lo : lo + step].astype(f32)
        for piece, weight in zip(pieces, weights):
            acc = acc + jnp.dot(piece[...], weight[:, lo : lo + step], preferred_element_type=f32)
        mid = acc.astype(bf16)
        middle[:, lo : lo + step] = mid
        mid = mid.astype(f32)
        total = total + jnp.sum(mid * mid, axis=1, keepdims=True)
    scale = lax.rsqrt(total * (1.0 / width) + norm_eps)
    for lo in range(0, width, step):
        mid = middle[:, lo : lo + step].astype(f32)
        normed[:, lo : lo + step] = (mid * scale * gain[:, lo : lo + step]).astype(bf16)


def out_norm(pieces, weights, resid, gain):
    count = len(pieces)
    vm = pl.BlockSpec(memory_space=pltpu.VMEM)
    shape = jax.ShapeDtypeStruct(resid.shape, bf16)
    return pl.pallas_call(
        functools.partial(out_norm_kernel, count),
        out_shape=(shape, shape),
        in_specs=[vm] * (2 * count + 2),
        out_specs=(vm, vm),
        compiler_params=pltpu.CompilerParams(vmem_limit_bytes=40 * 2**20),
        name="out_norm",
    )(*pieces, *weights, resid, gain.reshape(1, -1))


def expert_kernel(slots, peers, capacity, pad, *refs):
    pos = 0
    lines = refs[pos : pos + slots]
    pos += slots
    others = refs[pos : pos + slots * peers]
    pos += slots * peers
    ranks = refs[pos : pos + slots]
    pos += slots
    shares = refs[pos : pos + slots]
    pos += slots
    gate, up, down = refs[pos : pos + 3]
    pos += 3
    owns = refs[pos : pos + slots]
    pos += slots
    backs = refs[pos : pos + slots * peers]
    pos += slots * peers
    packed = refs[pos]
    expert = pl.program_id(0)
    rows = lines[0].shape[0]
    other_rows = others[0].shape[0]
    seat = lax.broadcasted_iota(jnp.int32, (pad, rows), 0).astype(f32)
    picks = [
        ranks[k][pl.ds(expert, 1), :] == jnp.where(seat < capacity, seat, -2.0) for k in range(slots)
    ]
    seat_row = lax.broadcasted_iota(jnp.int32, (pad, other_rows), 0)
    seat_col = lax.broadcasted_iota(jnp.int32, (pad, other_rows), 1)
    shift = (
        (seat_col == expert * capacity + seat_row) & (seat_row < capacity)
    ).astype(f32).astype(bf16)
    at = 0
    for k in range(slots):
        packed[at : at + pad, :] = jnp.dot(
            picks[k].astype(f32).astype(bf16), lines[k][...], preferred_element_type=f32
        ).astype(bf16)
        at += pad
        for j in range(peers):
            packed[at : at + pad, :] = jnp.dot(
                shift, others[k * peers + j][...], preferred_element_type=f32
            ).astype(bf16)
            at += pad
    tokens = packed[...]
    gated = jnp.dot(tokens, gate[0], preferred_element_type=f32)
    lifted = jnp.dot(tokens, up[0], preferred_element_type=f32)
    hidden = (gated * (1.0 / (1.0 + jnp.exp(-gated))) * lifted).astype(bf16)
    packed[...] = jnp.dot(hidden, down[0], preferred_element_type=f32).astype(bf16)
    at = 0
    first = expert == 0
    rows_in = (((0,), (0,)), ((), ()))
    for k in range(slots):
        mixing = jnp.where(picks[k], shares[k][pl.ds(expert, 1), :], 0.0).astype(bf16)
        part = lax.dot_general(
            mixing, packed[at : at + pad, :], rows_in, preferred_element_type=f32
        )
        owns[k][...] = jnp.where(first, part, owns[k][...] + part)
        at += pad
        for j in range(peers):
            part = lax.dot_general(
                shift, packed[at : at + pad, :], rows_in, preferred_element_type=f32
            ).astype(bf16)
            back = backs[k * peers + j]
            back[...] = jnp.where(first, part, back[...] + part)
            at += pad


def run_experts(lines, others, ranks, shares, gate, up, down, capacity):
    slots = len(lines)
    peers = len(others[0])
    experts, width, hidden = gate.shape
    pad = -(-capacity // 16) * 16
    flat = [o for group in others for o in group]

    def whole(a):
        return pl.BlockSpec(a.shape, lambda e: (0, 0), pipeline_mode=pl.Buffered(1))

    def per_expert(a):
        return pl.BlockSpec((1,) + a.shape[1:], lambda e: (e, 0, 0))

    own_shape = jax.ShapeDtypeStruct(lines[0].shape, f32)
    back_shape = jax.ShapeDtypeStruct(flat[0].shape, bf16)
    n_back = slots * peers
    total_rows = slots * (1 + peers) * pad
    outs = pl.pallas_call(
        functools.partial(expert_kernel, slots, peers, capacity, pad),
        grid=(experts,),
        out_shape=[own_shape] * slots + [back_shape] * n_back,
        in_specs=[whole(a) for a in (*lines, *flat, *ranks, *shares)]
        + [per_expert(a) for a in (gate, up, down)],
        out_specs=[whole(own_shape)] * slots + [whole(back_shape)] * n_back,
        scratch_shapes=[pltpu.VMEM((total_rows, width), bf16)],
        compiler_params=pltpu.CompilerParams(
            vmem_limit_bytes=58 * 2**20, dimension_semantics=("arbitrary",)
        ),
        cost_estimate=pl.CostEstimate(
            flops=6 * experts * total_rows * width * hidden,
            bytes_accessed=6 * experts * width * hidden,
            transcendentals=experts * total_rows * hidden,
        ),
        name="experts",
    )(*lines, *flat, *ranks, *shares, gate, up, down)
    owns = outs[:slots]
    backs = [outs[slots + k * peers : slots + (k + 1) * peers] for k in range(slots)]
    return owns, backs


def shards(
    resid,
    pool_in,
    pool_weight,
    pool_scale,
    out_weight,
    norm_gain,
    route_ids,
    route_weight,
    expert_gate,
    expert_up,
    expert_down,
    shared_gate,
    shared_up,
    shared_down,
):
    n_sp, n_tp = lax.axis_size("sp"), lax.axis_size("tp")
    inner = n_sp // outer
    plane = lax.axis_index("sp") // inner
    lane = lax.axis_index("sp") % inner
    mine = lax.axis_index("tp")
    rows_here, top_count = route_ids.shape
    experts_here = expert_gate.shape[0]
    expert_total = experts_here * n_sp
    capacity = rows_here * top_count * 3 // (2 * expert_total)

    def along_outer(x, pairs):
        return lax.ppermute(
            x, "sp", [(a * inner + i, b * inner + i) for a, b in pairs for i in range(inner)]
        )

    def along_inner(x, by):
        return lax.ppermute(
            x,
            "sp",
            [
                (a * inner + i, a * inner + (i + by) % inner)
                for a in range(outer)
                for i in range(inner)
            ],
        )

    def along_tp(x, bits):
        return lax.ppermute(x, "tp", [(i, i ^ bits) for i in range(n_tp)])

    weights = [out_weight, along_tp(out_weight, 1), along_tp(out_weight, 2)]
    weights.append(along_tp(weights[2], 1))

    ids = route_ids.T
    chosen = route_weight.T
    numbers = lax.iota(jnp.int32, expert_total)[:, None]
    member = jnp.zeros((expert_total, rows_here), jnp.bool_)
    share = jnp.zeros((expert_total, rows_here), f32)
    for k in range(top_count):
        hit = ids[k][None, :] == numbers
        member = member | hit
        share = share + jnp.where(hit, chosen[k][None, :], 0.0)
    order = lax.iota(jnp.int32, rows_here)
    ahead = (order[:, None] < order[None, :]).astype(bf16)
    seat = jnp.dot(member.astype(bf16), ahead, preferred_element_type=f32)
    seat = jnp.where(member, seat, -1.0)
    per_plane = inner * experts_here
    table = jnp.stack(
        [seat.reshape(outer, per_plane, rows_here), share.reshape(outer, per_plane, rows_here)],
        axis=1,
    )

    def table_for(index):
        return lax.dynamic_index_in_dim(table, index, axis=0, keepdims=False)

    tables = [table_for(plane)]
    for by in range(1, outer):
        tables.append(
            along_outer(
                table_for((plane + by) % outer), [(a, (a + by) % outer) for a in range(outer)]
            )
        )
    low = plane <= 1
    slot_tables = [
        tables[0],
        jnp.where(low, tables[3], tables[1]),
        tables[2],
        jnp.where(low, tables[1], tables[3]),
    ]

    def group_of(slot, by):
        start = ((lane + by) % inner) * experts_here
        return lax.dynamic_slice_in_dim(slot_tables[slot], start, experts_here, axis=1)

    slots = range(4)
    peers = range(1, inner)
    own_tables = [group_of(k, 0) for k in slots]
    ranks = [t[0] for t in own_tables]
    shares = [t[1] for t in own_tables]
    seats_out = experts_here * capacity
    line_no = lax.iota(jnp.int32, seats_out)
    spreader = (
        (line_no // capacity)[:, None] == lax.iota(jnp.int32, experts_here)[None, :]
    ).astype(bf16)
    seat_no = (line_no % capacity).astype(f32)[:, None]
    send_pick, send_mix = [], []
    for k in slots:
        send_pick.append([])
        send_mix.append([])
        for j in peers:
            t = group_of(k, j).astype(bf16)
            wide_rank = jnp.dot(spreader, t[0], preferred_element_type=f32)
            wide_share = jnp.dot(spreader, t[1], preferred_element_type=f32)
            hit = wide_rank == seat_no
            send_pick[k].append(hit.astype(bf16))
            send_mix[k].append(jnp.where(hit, wide_share, 0.0).astype(bf16))

    pooled = pool_mix(pool_in, pool_weight, pool_scale)

    def pooled_for(index):
        return lax.dynamic_slice_in_dim(pooled, index * rows_here, rows_here, axis=0)

    pieces = [pooled_for(mine)] + [along_tp(pooled_for(mine ^ b), b) for b in range(1, n_tp)]
    middle, normed = out_norm(pieces, weights, resid, norm_gain)

    up1 = along_outer(normed, [(0, 1), (1, 2), (2, 3)])
    down1 = along_outer(normed, [(1, 0), (2, 1), (3, 2)])
    up2 = along_outer(up1, [(1, 2), (2, 3)])
    down2 = along_outer(down1, [(1, 0), (2, 1)])
    up3 = along_outer(up2, [(2, 3)])
    down3 = along_outer(down2, [(1, 0)])
    lines = [
        normed,
        jnp.where(low, down1, up1),
        jnp.where(low, down2, up2),
        jnp.where(plane == 1, up1, jnp.where(plane == 2, down1, jnp.where(low, down3, up3))),
    ]

    def exchange(k):
        return [
            along_inner(
                jnp.dot(send_pick[k][j - 1], lines[k], preferred_element_type=f32).astype(bf16), j
            )
            for j in peers
        ]

    arrived = [exchange(k) for k in slots]
    owns, backs = [None] * 4, [None] * 4
    for batch in ((0, 1), (2,), (3,)):
        got_own, got_back = run_experts(
            [lines[k] for k in batch],
            [arrived[k] for k in batch],
            [ranks[k] for k in batch],
            [shares[k] for k in batch],
            expert_gate,
            expert_up,
            expert_down,
            capacity,
        )
        for i, k in enumerate(batch):
            owns[k], backs[k] = got_own[i], got_back[i]

    def partial_sum(k):
        total = owns[k]
        for j in peers:
            q = along_inner(backs[k][j - 1], -j)
            total = total + lax.dot_general(
                send_mix[k][j - 1], q, (((0,), (0,)), ((), ())), preferred_element_type=f32
            )
        return total

    sums = {k: partial_sum(k) for k in (3, 2, 1, 0)}

    shared_hidden = (
        jax.nn.silu(jnp.dot(normed, shared_gate, preferred_element_type=f32))
        * jnp.dot(normed, shared_up, preferred_element_type=f32)
    ).astype(bf16)
    shared_out = jnp.dot(shared_hidden, shared_down, preferred_element_type=f32)

    far = sums[3].astype(bf16)
    got_up = along_outer(far, [(0, 1)])
    got_down = along_outer(far, [(3, 2)])
    mid = (sums[2] + got_up.astype(f32) + got_down.astype(f32)).astype(bf16)
    got_up = along_outer(mid, [(0, 1), (1, 2)])
    got_down = along_outer(mid, [(3, 2), (2, 1)])
    near_up = (jnp.where(plane == 2, sums[3], sums[1]) + got_up.astype(f32)).astype(bf16)
    near_down = (jnp.where(plane == 1, sums[3], sums[1]) + got_down.astype(f32)).astype(bf16)
    got_up = along_outer(near_up, [(0, 1), (1, 2), (2, 3)])
    got_down = along_outer(near_down, [(3, 2), (2, 1), (1, 0)])
    return (
        middle.astype(f32) + shared_out + sums[0] + got_up.astype(f32) + got_down.astype(f32)
    ).astype(bf16)


def solution(mesh):
    return jax.shard_map(
        shards,
        mesh=mesh,
        in_specs=(
            P(("sp", "tp"), None),
            P("sp", "tp"),
            P("tp", None, None),
            P("tp"),
            P("tp", None),
            P(),
            P(("sp", "tp"), None),
            P(("sp", "tp"), None),
            P("sp", None, None),
            P("sp", None, None),
            P("sp", None, None),
            P(),
            P(),
            P(),
        ),
        out_specs=P(("sp", "tp"), None),
        check_vma=False,
    )
```

```python
import functools

import jax
import jax.numpy as jnp
from jax import lax
from jax.experimental import pallas as pl
from jax.experimental.pallas import tpu as pltpu
from jax.sharding import PartitionSpec as P


reach_rows = 8
norm_eps = 1e-06
outer = 4


f32 = jnp.float32
bf16 = jnp.bfloat16


def with_halo(cells, axis, width):
    count = lax.axis_size(axis)
    ends = count - 1
    head = cells[:width]
    tail = cells[cells.shape[0] - width :]
    return jnp.concatenate(
        [
            lax.ppermute(tail, axis, [(i, i + 1) for i in range(ends)]),
            cells,
            lax.ppermute(head, axis, [(i + 1, i) for i in range(ends)]),
        ],
        axis=0,
    )


def window_means(padded, length, offset, whole_len):
    positions = offset + lax.iota(jnp.int32, length)
    running = jnp.zeros((length,) + padded.shape[1:], f32)
    averages = []
    covered = 0
    for section_num in range(4):
        half_span = 2**section_num
        for row_shift in list(range(-half_span, -covered)) + list(range(covered, half_span)):
            running = running + padded[reach_rows + row_shift : reach_rows + row_shift + length]
        covered = half_span
        upper_end = jnp.minimum(positions + half_span, whole_len)
        lower_end = jnp.maximum(positions - half_span, 0)
        row_count = (upper_end - lower_end).astype(f32)
        averages.append(running / row_count[:, None, None])
    return averages


def pool_mix(pool_in, pool_weight, pool_scale):
    tok_local = pool_in.shape[0]
    local_groups, group_width = pool_weight.shape[:2]
    padded = with_halo(pool_in, "sp", reach_rows).astype(f32)
    padded = padded.reshape(tok_local + 2 * reach_rows, local_groups, group_width)
    averages = window_means(
        padded, tok_local, lax.axis_index("sp") * tok_local, tok_local * lax.axis_size("sp")
    )
    center = padded[reach_rows : reach_rows + tok_local]
    group_ids = lax.axis_index("tp") * local_groups + lax.iota(jnp.int32, local_groups)
    chosen = averages[0]
    for section_num in range(1, 4):
        chosen = jnp.where((group_ids == section_num)[None, :, None], averages[section_num], chosen)
    spread = (chosen - center).astype(bf16)
    mixed_rows = jnp.einsum("tgc,gce->tge", spread, pool_weight, preferred_element_type=f32)
    return (mixed_rows.reshape(tok_local, -1) * pool_scale[None, :]).astype(bf16)


def out_norm_kernel(blocks, keep, pick, *refs):
    plane, refs = refs[0], refs[1:]
    pools, resids = refs[:blocks], refs[blocks : 2 * blocks]
    refs = refs[2 * blocks :]
    gain, weights, outs = refs[0], refs[1:5], refs[5:]
    width = gain.shape[1]
    depth = weights[0].shape[0]
    step = 1024
    steps = width // step

    def part(n):
        return pl.ds(pl.multiple_of(n * step, step), step)

    for i in range(blocks):
        pool, resid = pools[i], resids[i]
        normed = outs[i]
        middle = outs[blocks] if keep and i == 0 else normed

        def project(n, total):
            at = part(n)
            acc = resid[:, at].astype(f32)
            for j, weight in enumerate(weights):
                acc = acc + jnp.dot(
                    pool[:, j * depth : (j + 1) * depth],
                    weight[:, at],
                    preferred_element_type=f32,
                )
            mid = acc.astype(bf16)
            middle[:, at] = mid
            mid = mid.astype(f32)
            return total + jnp.sum(mid * mid, axis=1, keepdims=True)

        total = lax.fori_loop(0, steps, project, jnp.zeros((resid.shape[0], 1), f32))
        scale = lax.rsqrt(total * (1.0 / width) + norm_eps)

        def finish(n, carry):
            at = part(n)
            value = (middle[:, at].astype(f32) * scale * gain[:, at]).astype(bf16)
            normed[:, at] = value
            if pick:
                near, spare = outs[blocks], outs[blocks + 1]
                low = plane[0] <= 1

                @pl.when(low if i == 1 else jnp.logical_not(low))
                def _():
                    near[:, at] = value

                @pl.when(plane[0] == 1 + i)
                def _():
                    spare[:, at] = value

                if i == 0:

                    @pl.when((plane[0] != 1) & (plane[0] != 2))
                    def _():
                        spare[:, at] = jnp.zeros_like(value)

            return carry

        lax.fori_loop(0, steps, finish, 0)


def out_norm(pools, resids, gain, weights, plane, keep, pick):
    blocks = len(pools)
    vm = pl.BlockSpec(memory_space=pltpu.VMEM)
    shapes = [jax.ShapeDtypeStruct(r.shape, bf16) for r in resids]
    shapes += [shapes[0]] * (1 if keep else 2 if pick else 0)
    rows = sum(r.shape[0] for r in resids)
    return pl.pallas_call(
        functools.partial(out_norm_kernel, blocks, keep, pick),
        out_shape=shapes,
        in_specs=[pl.BlockSpec(memory_space=pltpu.SMEM)]
        + [vm] * (2 * blocks + 1 + len(weights)),
        out_specs=[vm] * len(shapes),
        compiler_params=pltpu.CompilerParams(vmem_limit_bytes=40 * 2**20),
        cost_estimate=pl.CostEstimate(
            flops=2 * rows * pools[0].shape[1] * gain.shape[0],
            bytes_accessed=4 * rows * gain.shape[0],
            transcendentals=rows,
        ),
        name="out_norm",
    )(plane.reshape(1), *pools, *resids, gain.reshape(1, -1), *weights)


def combine_kernel(count, own, *refs):
    mixes, parts, out = refs[:count], refs[count : 2 * count], refs[2 * count]
    total = own[...]
    for mix, part in zip(mixes, parts):
        total = total + lax.dot_general(
            mix[...], part[...], (((0,), (0,)), ((), ())), preferred_element_type=f32
        )
    out[...] = total.astype(bf16)


def combine(own, mixes, parts):
    count = len(parts)
    rows, width = own.shape
    step = width // 4
    whole = [pl.BlockSpec(m.shape, lambda n: (0, 0)) for m in mixes]
    cut = [pl.BlockSpec((p.shape[0], step), lambda n: (0, n)) for p in parts]
    mine = pl.BlockSpec((rows, step), lambda n: (0, n))
    return pl.pallas_call(
        functools.partial(combine_kernel, count),
        grid=(4,),
        out_shape=jax.ShapeDtypeStruct(own.shape, bf16),
        in_specs=[mine] + whole + cut,
        out_specs=mine,
        compiler_params=pltpu.CompilerParams(vmem_limit_bytes=24 * 2**20),
        cost_estimate=pl.CostEstimate(
            flops=2 * rows * width * sum(p.shape[0] for p in parts),
            bytes_accessed=8 * rows * width,
            transcendentals=0,
        ),
        name="combine",
    )(own, *mixes, *parts)


def expert_kernel(peers, capacity, pad, *refs):
    line, others, refs = refs[0], refs[1 : 1 + peers], refs[1 + peers :]
    rank, share, gate, up, down, own = refs[:6]
    backs = refs[6 : 6 + peers]
    packed, made, pick, mixing, shift = refs[6 + peers :]
    expert = pl.program_id(0)
    count = pl.num_programs(0)
    experts = rank.shape[0]
    rows = line.shape[0]
    other_rows = others[0].shape[0]

    @pl.when(expert == 0)
    def _():
        seat = lax.broadcasted_iota(jnp.int32, (pad, rows), 0).astype(f32)
        seat = jnp.where(seat < capacity, seat, -2.0)
        row = lax.broadcasted_iota(jnp.int32, (pad, other_rows), 0)
        col = lax.broadcasted_iota(jnp.int32, (pad, other_rows), 1)
        for e in range(experts):
            here = slice(e * pad, (e + 1) * pad)
            hit = rank[e : e + 1, :] == seat
            pick[here, :] = hit.astype(f32).astype(bf16)
            mixing[here, :] = jnp.where(hit, share[e : e + 1, :], 0.0).astype(bf16)
            shift[here, :] = (
                ((col == e * capacity + row) & (row < capacity)).astype(f32).astype(bf16)
            )
        for i in range(1 + peers):
            if i == 0:
                moved = jnp.dot(pick[...], line[...], preferred_element_type=f32)
            else:
                moved = jnp.dot(shift[...], others[i - 1][...], preferred_element_type=f32)
            moved = moved.astype(bf16)
            for e in range(experts):
                packed[e, i * pad : (i + 1) * pad, :] = moved[e * pad : (e + 1) * pad]

    tokens = packed[expert]
    gated = jnp.dot(tokens, gate[0], preferred_element_type=f32)
    lifted = jnp.dot(tokens, up[0], preferred_element_type=f32)
    hidden = (gated * (1.0 / (1.0 + jnp.exp(-gated))) * lifted).astype(bf16)
    result = jnp.dot(hidden, down[0], preferred_element_type=f32).astype(bf16)
    for i in range(1 + peers):
        made[i, pl.ds(pl.multiple_of(expert * pad, pad), pad), :] = result[i * pad : (i + 1) * pad]

    @pl.when(expert == count - 1)
    def _():
        rows_in = (((0,), (0,)), ((), ()))
        own[...] = lax.dot_general(mixing[...], made[0], rows_in, preferred_element_type=f32)
        for j in range(peers):
            backs[j][...] = lax.dot_general(
                shift[...], made[1 + j], rows_in, preferred_element_type=f32
            ).astype(bf16)


def run_experts(line, others, rank, share, gate, up, down, capacity):
    peers = len(others)
    experts, width, hidden = gate.shape
    pad = -(-capacity // 16) * 16
    rows = line.shape[0]
    vm = pl.BlockSpec(memory_space=pltpu.VMEM)

    def per_expert(a):
        return pl.BlockSpec((1,) + a.shape[1:], lambda e: (e, 0, 0))

    back_shape = jax.ShapeDtypeStruct(others[0].shape, bf16)
    filled = (1 + peers) * pad
    outs = pl.pallas_call(
        functools.partial(expert_kernel, peers, capacity, pad),
        grid=(experts,),
        out_shape=[jax.ShapeDtypeStruct(line.shape, f32)] + [back_shape] * peers,
        in_specs=[vm] * (3 + peers) + [per_expert(a) for a in (gate, up, down)],
        out_specs=[vm] * (1 + peers),
        scratch_shapes=[
            pltpu.VMEM((experts, filled, width), bf16),
            pltpu.VMEM((1 + peers, experts * pad, width), bf16),
            pltpu.VMEM((experts * pad, rows), bf16),
            pltpu.VMEM((experts * pad, rows), bf16),
            pltpu.VMEM((experts * pad, others[0].shape[0]), bf16),
        ],
        compiler_params=pltpu.CompilerParams(
            vmem_limit_bytes=48 * 2**20, dimension_semantics=("arbitrary",)
        ),
        cost_estimate=pl.CostEstimate(
            flops=6 * experts * filled * width * hidden,
            bytes_accessed=6 * experts * width * hidden,
            transcendentals=experts * filled * hidden,
        ),
        name="experts",
    )(line, *others, rank, share, gate, up, down)
    return outs[0], outs[1:]


def shards(
    resid,
    pool_in,
    pool_weight,
    pool_scale,
    out_weight,
    norm_gain,
    route_ids,
    route_weight,
    expert_gate,
    expert_up,
    expert_down,
    shared_gate,
    shared_up,
    shared_down,
):
    n_sp, n_tp = lax.axis_size("sp"), lax.axis_size("tp")
    inner = n_sp // outer
    plane = lax.axis_index("sp") // inner
    lane = lax.axis_index("sp") % inner
    mine = lax.axis_index("tp")
    rows_here, top_count = route_ids.shape
    experts_here = expert_gate.shape[0]
    expert_total = experts_here * n_sp
    capacity = rows_here * top_count * 3 // (2 * expert_total)

    def along_outer(x, pairs):
        pairs = [(a * inner + i, b * inner + i) for a, b in pairs for i in range(inner)]
        return lax.ppermute(x, "sp", pairs)

    def along_inner(x, by):
        pairs = [
            (a * inner + i, a * inner + (i + by) % inner)
            for a in range(outer)
            for i in range(inner)
        ]
        return lax.ppermute(x, "sp", pairs)

    def along_tp(x, bits):
        return lax.ppermute(x, "tp", [(i, i ^ bits) for i in range(n_tp)])

    ups = [(0, 1), (1, 2), (2, 3)]
    downs = [(3, 2), (2, 1), (1, 0)]

    weights = [out_weight, along_tp(out_weight, 1), along_tp(out_weight, 2)]
    weights.append(along_tp(weights[2], 1))
    resid_up = along_outer(resid, ups)
    resid_down = along_outer(resid, downs)

    ids = route_ids.T
    chosen = route_weight.T
    numbers = lax.iota(jnp.int32, expert_total)[:, None]
    member = jnp.zeros((expert_total, rows_here), jnp.bool_)
    share = jnp.zeros((expert_total, rows_here), f32)
    for k in range(top_count):
        hit = ids[k][None, :] == numbers
        member = member | hit
        share = share + jnp.where(hit, chosen[k][None, :], 0.0)
    order = lax.iota(jnp.int32, rows_here)
    ahead = (order[:, None] < order[None, :]).astype(bf16)
    seat = jnp.dot(member.astype(bf16), ahead, preferred_element_type=f32)
    seat = jnp.where(member, seat, -1.0)
    per_plane = inner * experts_here
    table = jnp.stack(
        [seat.reshape(outer, per_plane, rows_here), share.reshape(outer, per_plane, rows_here)],
        axis=1,
    )

    def table_for(by):
        return lax.dynamic_index_in_dim(table, lax.rem(plane + by, outer), axis=0, keepdims=False)

    tables = [table_for(0)]
    for by in range(1, outer):
        tables.append(along_outer(table_for(by), [(a, (a + by) % outer) for a in range(outer)]))
    low = plane <= 1
    slot_tables = [
        tables[0],
        jnp.where(low, tables[3], tables[1]),
        tables[2],
        jnp.where(low, tables[1], tables[3]),
    ]
    slots = range(4)
    peers = range(1, inner)

    def group_of(slot, by):
        start = lax.rem(lane + by, inner) * experts_here
        return lax.dynamic_slice_in_dim(slot_tables[slot], start, experts_here, axis=1)

    seats_out = experts_here * capacity
    line_no = lax.iota(jnp.int32, seats_out)
    spreader = (
        lax.div(line_no, capacity)[:, None] == lax.iota(jnp.int32, experts_here)[None, :]
    ).astype(bf16)
    seat_no = lax.rem(line_no, capacity).astype(f32)[:, None]
    send_pick = [[] for _ in slots]
    send_mix = [[] for _ in slots]
    for k in slots:
        for j in peers:
            t = group_of(k, j).astype(bf16)
            wide_rank = jnp.dot(spreader, t[0], preferred_element_type=f32)
            wide_share = jnp.dot(spreader, t[1], preferred_element_type=f32)
            hit = wide_rank == seat_no
            send_pick[k].append(hit.astype(bf16))
            send_mix[k].append(jnp.where(hit, wide_share, 0.0).astype(bf16))

    def exchange(slot, rows):
        got = []
        for j in peers:
            sent = jnp.dot(send_pick[slot][j - 1], rows, preferred_element_type=f32).astype(bf16)
            got.append(along_inner(sent, j))
        return got

    other_resid = exchange(0, resid)

    pooled = pool_mix(pool_in, pool_weight, pool_scale)

    def pooled_for(bits):
        return lax.dynamic_slice_in_dim(pooled, (mine ^ bits) * rows_here, rows_here, axis=0)

    pieces = [pooled_for(0)] + [along_tp(pooled_for(b), b) for b in range(1, n_tp)]
    pooled = jnp.concatenate(pieces, axis=1)
    pooled_up = along_outer(pooled, ups)
    pooled_down = along_outer(pooled, downs)
    other_pooled = exchange(0, pooled)

    up1, down1, near, spare = out_norm(
        [pooled_up, pooled_down],
        [resid_up, resid_down],
        norm_gain,
        weights,
        plane,
        False,
        True,
    )
    normed, *other_normed, middle = out_norm(
        [pooled, *other_pooled], [resid, *other_resid], norm_gain, weights, plane, True, False
    )

    up2 = along_outer(up1, ups[1:])
    down2 = along_outer(down1, downs[1:])
    up3 = along_outer(up2, ups[2:])
    down3 = along_outer(down2, downs[2:])
    lines = [normed, near, up2 + down2, spare + up3 + down3]
    arrived = [other_normed] + [exchange(k, lines[k]) for k in (1, 2, 3)]
    owns, backs = [], []
    for k in slots:
        own_table = group_of(k, 0)
        own, back = run_experts(
            lines[k],
            arrived[k],
            own_table[0],
            own_table[1],
            expert_gate,
            expert_up,
            expert_down,
            capacity,
        )
        owns.append(own)
        backs.append(back)

    def partial_sum(k):
        parts = [along_inner(backs[k][j - 1], -j) for j in peers]
        return combine(owns[k], send_mix[k], parts)

    sums = [partial_sum(k) for k in slots]

    shared_hidden = (
        jax.nn.silu(jnp.dot(normed, shared_gate, preferred_element_type=f32))
        * jnp.dot(normed, shared_up, preferred_element_type=f32)
    ).astype(bf16)
    base = middle.astype(f32) + jnp.dot(
        shared_hidden, shared_down, preferred_element_type=f32
    )

    got_up = along_outer(sums[3], ups[:1])
    got_down = along_outer(sums[3], downs[:1])
    mid = sums[2] + got_up + got_down
    got_up = along_outer(mid, ups[:2])
    got_down = along_outer(mid, downs[:2])
    near_up = jnp.where(plane == 2, sums[3], sums[1]) + got_up
    near_down = jnp.where(plane == 1, sums[3], sums[1]) + got_down
    got_up = along_outer(near_up, ups)
    got_down = along_outer(near_down, downs)
    base = base + sums[0].astype(f32)
    return (base + got_up.astype(f32) + got_down.astype(f32)).astype(bf16)


def solution(mesh):
    return jax.shard_map(
        shards,
        mesh=mesh,
        in_specs=(
            P(("sp", "tp"), None),
            P("sp", "tp"),
            P("tp", None, None),
            P("tp"),
            P("tp", None),
            P(),
            P(("sp", "tp"), None),
            P(("sp", "tp"), None),
            P("sp", None, None),
            P("sp", None, None),
            P("sp", None, None),
            P(),
            P(),
            P(),
        ),
        out_specs=P(("sp", "tp"), None),
        check_vma=False,
    )
```

```python
import functools

import jax
import jax.numpy as jnp
from jax import lax
from jax.experimental import pallas as pl
from jax.experimental.pallas import tpu as pltpu
from jax.sharding import PartitionSpec as P


reach_rows = 8
norm_eps = 1e-06
outer = 4


f32 = jnp.float32
bf16 = jnp.bfloat16


def with_halo(cells, axis, width):
    count = lax.axis_size(axis)
    ends = count - 1
    head = cells[:width]
    tail = cells[cells.shape[0] - width :]
    return jnp.concatenate(
        [
            lax.ppermute(tail, axis, [(i, i + 1) for i in range(ends)]),
            cells,
            lax.ppermute(head, axis, [(i + 1, i) for i in range(ends)]),
        ],
        axis=0,
    )


def window_means(padded, length, offset, whole_len):
    positions = offset + lax.iota(jnp.int32, length)
    running = jnp.zeros((length,) + padded.shape[1:], f32)
    averages = []
    covered = 0
    for section_num in range(4):
        half_span = 2**section_num
        for row_shift in list(range(-half_span, -covered)) + list(range(covered, half_span)):
            running = running + padded[reach_rows + row_shift : reach_rows + row_shift + length]
        covered = half_span
        upper_end = jnp.minimum(positions + half_span, whole_len)
        lower_end = jnp.maximum(positions - half_span, 0)
        row_count = (upper_end - lower_end).astype(f32)
        averages.append(running / row_count[:, None, None])
    return averages


def pool_mix(pool_in, pool_weight, pool_scale):
    tok_local = pool_in.shape[0]
    local_groups, group_width = pool_weight.shape[:2]
    padded = with_halo(pool_in, "sp", reach_rows).astype(f32)
    padded = padded.reshape(tok_local + 2 * reach_rows, local_groups, group_width)
    averages = window_means(
        padded, tok_local, lax.axis_index("sp") * tok_local, tok_local * lax.axis_size("sp")
    )
    center = padded[reach_rows : reach_rows + tok_local]
    group_ids = lax.axis_index("tp") * local_groups + lax.iota(jnp.int32, local_groups)
    chosen = averages[0]
    for section_num in range(1, 4):
        chosen = jnp.where((group_ids == section_num)[None, :, None], averages[section_num], chosen)
    spread = (chosen - center).astype(bf16)
    mixed_rows = jnp.einsum("tgc,gce->tge", spread, pool_weight, preferred_element_type=f32)
    return (mixed_rows.reshape(tok_local, -1) * pool_scale[None, :]).astype(bf16)


def out_norm_kernel(blocks, keep, halved, *refs):
    pools, resids = refs[:blocks], refs[blocks : 2 * blocks]
    refs = refs[2 * blocks :]
    gain, refs = refs[0], refs[1:]
    weights = []
    for parts in halved:
        weights.append(refs[:parts])
        refs = refs[parts:]
    outs = refs
    width = gain.shape[1]
    depth = weights[0][0].shape[0]
    step = 1024
    steps = width // step

    def part(n):
        return pl.ds(pl.multiple_of(n * step, step), step)

    for i in range(blocks):
        pool, resid = pools[i], resids[i]
        normed = outs[i]
        middle = outs[blocks] if keep and i == 0 else normed

        def project(half, n, total):
            at = part(n + half * (steps // 2))
            acc = resid[:, at].astype(f32)
            for j, weight in enumerate(weights):
                rows = weight[half][:, part(n)] if len(weight) == 2 else weight[0][:, at]
                acc = acc + jnp.dot(
                    pool[:, j * depth : (j + 1) * depth], rows, preferred_element_type=f32
                )
            mid = acc.astype(bf16)
            middle[:, at] = mid
            mid = mid.astype(f32)
            return total + jnp.sum(mid * mid, axis=1, keepdims=True)

        total = jnp.zeros((resid.shape[0], 1), f32)
        for half in range(2):
            total = lax.fori_loop(0, steps // 2, functools.partial(project, half), total)
        scale = lax.rsqrt(total * (1.0 / width) + norm_eps)

        def finish(n, carry):
            at = part(n)
            normed[:, at] = (middle[:, at].astype(f32) * scale * gain[:, at]).astype(bf16)
            return carry

        lax.fori_loop(0, steps, finish, 0)


def out_norm(pools, resids, gain, weights, keep):
    blocks = len(pools)
    vm = pl.BlockSpec(memory_space=pltpu.VMEM)
    shapes = [jax.ShapeDtypeStruct(r.shape, bf16) for r in resids]
    shapes += [shapes[0]] * (1 if keep else 0)
    rows = sum(r.shape[0] for r in resids)
    flat = [w for group in weights for w in group]
    return pl.pallas_call(
        functools.partial(out_norm_kernel, blocks, keep, [len(g) for g in weights]),
        out_shape=shapes,
        in_specs=[vm] * (2 * blocks + 1 + len(flat)),
        out_specs=[vm] * len(shapes),
        compiler_params=pltpu.CompilerParams(vmem_limit_bytes=36 * 2**20),
        cost_estimate=pl.CostEstimate(
            flops=2 * rows * pools[0].shape[1] * gain.shape[0],
            bytes_accessed=4 * rows * gain.shape[0],
            transcendentals=rows,
        ),
        name="out_norm",
    )(*pools, *resids, gain.reshape(1, -1), *flat)


def combine_kernel(count, own, *refs):
    mixes, parts, out = refs[:count], refs[count : 2 * count], refs[2 * count]
    total = own[...]
    for mix, part in zip(mixes, parts):
        total = total + lax.dot_general(
            mix[...], part[...], (((0,), (0,)), ((), ())), preferred_element_type=f32
        )
    out[...] = total.astype(bf16)


def combine(own, mixes, parts, half):
    count = len(parts)
    rows, width = own.shape
    step = width // 4
    skip = 2 * half
    cut_parts = parts[0].shape[1] == width
    whole = [pl.BlockSpec(m.shape, lambda n: (0, 0)) for m in mixes]
    cut = [
        pl.BlockSpec((p.shape[0], step), lambda n: (0, n + (skip if cut_parts else 0)))
        for p in parts
    ]
    return pl.pallas_call(
        functools.partial(combine_kernel, count),
        grid=(2,),
        out_shape=jax.ShapeDtypeStruct((rows, width // 2), bf16),
        in_specs=[pl.BlockSpec((rows, step), lambda n: (0, n + skip))] + whole + cut,
        out_specs=pl.BlockSpec((rows, step), lambda n: (0, n)),
        compiler_params=pltpu.CompilerParams(vmem_limit_bytes=24 * 2**20),
        cost_estimate=pl.CostEstimate(
            flops=rows * width * sum(p.shape[0] for p in parts),
            bytes_accessed=4 * rows * width,
            transcendentals=0,
        ),
        name="combine",
    )(own, *mixes, *parts)


def finish_kernel(base, own_a, own_b, up_a, up_b, down_a, down_b, out):
    span = own_a.shape[1]
    for h, group in enumerate(((own_a, up_a, down_a), (own_b, up_b, down_b))):
        at = slice(h * span, (h + 1) * span)
        total = base[:, at]
        for part in group:
            total = total + part[...].astype(f32)
        out[:, at] = total.astype(bf16)


def finish(base, *parts):
    vm = pl.BlockSpec(memory_space=pltpu.VMEM)
    return pl.pallas_call(
        finish_kernel,
        out_shape=jax.ShapeDtypeStruct(base.shape, bf16),
        in_specs=[vm] * (1 + len(parts)),
        out_specs=vm,
        compiler_params=pltpu.CompilerParams(vmem_limit_bytes=20 * 2**20),
        name="finish",
    )(base, *parts)


def expert_kernel(peers, parts, capacity, pad, *refs):
    line, refs = refs[:parts], refs[parts:]
    others = [refs[j * parts : (j + 1) * parts] for j in range(peers)]
    refs = refs[peers * parts :]
    rank, share, gate, up, down, own = refs[:6]
    backs = [refs[6 + j * parts : 6 + (j + 1) * parts] for j in range(peers)]
    packed, made, pick, mixing, shift = refs[6 + peers * parts :]
    expert = pl.program_id(0)
    count = pl.num_programs(0)
    experts = rank.shape[0]
    rows, span = line[0].shape
    other_rows = others[0][0].shape[0]
    step = 1024

    @pl.when(expert == 0)
    def _():
        seat = lax.broadcasted_iota(jnp.int32, (pad, rows), 0).astype(f32)
        seat = jnp.where(seat < capacity, seat, -2.0)
        row = lax.broadcasted_iota(jnp.int32, (pad, other_rows), 0)
        col = lax.broadcasted_iota(jnp.int32, (pad, other_rows), 1)
        for e in range(experts):
            here = slice(e * pad, (e + 1) * pad)
            hit = rank[e : e + 1, :] == seat
            pick[here, :] = hit.astype(f32).astype(bf16)
            mixing[here, :] = jnp.where(hit, share[e : e + 1, :], 0.0).astype(bf16)
            shift[here, :] = (
                ((col == e * capacity + row) & (row < capacity)).astype(f32).astype(bf16)
            )
        for h in range(parts):

            def gather(n, carry):
                at = pl.ds(pl.multiple_of(n * step, step), step)
                to = pl.ds(pl.multiple_of(h * span + n * step, step), step)
                for i in range(1 + peers):
                    source, chooser = (line, pick) if i == 0 else (others[i - 1], shift)
                    moved = jnp.dot(
                        chooser[...], source[h][:, at], preferred_element_type=f32
                    ).astype(bf16)
                    for e in range(experts):
                        packed[e, i * pad : (i + 1) * pad, to] = moved[e * pad : (e + 1) * pad]
                return carry

            lax.fori_loop(0, span // step, gather, 0)

    width = packed.shape[2]
    wide = gate.shape[2]
    filled = packed.shape[1]

    def project(n, carry):
        at = pl.ds(pl.multiple_of(n * step, step), step)
        tokens = packed[expert, :, at]
        return (
            carry[0] + jnp.dot(tokens, gate[0, at, :], preferred_element_type=f32),
            carry[1] + jnp.dot(tokens, up[0, at, :], preferred_element_type=f32),
        )

    zero = jnp.zeros((filled, wide), f32)
    gated, lifted = lax.fori_loop(0, width // step, project, (zero, zero))
    hidden = (gated * (1.0 / (1.0 + jnp.exp(-gated))) * lifted).astype(bf16)

    def lower(n, carry):
        at = pl.ds(pl.multiple_of(n * step, step), step)
        result = jnp.dot(hidden, down[0, :, at], preferred_element_type=f32).astype(bf16)
        for i in range(1 + peers):
            made[i, pl.ds(pl.multiple_of(expert * pad, pad), pad), at] = result[
                i * pad : (i + 1) * pad
            ]
        return carry

    lax.fori_loop(0, width // step, lower, 0)

    @pl.when(expert == count - 1)
    def _():
        rows_in = (((0,), (0,)), ((), ()))
        for h in range(parts):

            def spread(n, carry):
                at = pl.ds(pl.multiple_of(n * step, step), step)
                come = pl.ds(pl.multiple_of(h * span + n * step, step), step)
                own[:, come] = lax.dot_general(
                    mixing[...], made[0, :, come], rows_in, preferred_element_type=f32
                )
                for j in range(peers):
                    backs[j][h][:, at] = lax.dot_general(
                        shift[...], made[1 + j, :, come], rows_in, preferred_element_type=f32
                    ).astype(bf16)
                return carry

            lax.fori_loop(0, span // step, spread, 0)


def run_experts(line, others, rank, share, gate, up, down, capacity):
    peers = len(others)
    parts = len(line)
    experts, width, hidden = gate.shape
    pad = -(-capacity // 16) * 16
    rows = line[0].shape[0]
    vm = pl.BlockSpec(memory_space=pltpu.VMEM)
    flat = [h for group in others for h in group]

    def per_expert(a):
        return pl.BlockSpec((1,) + a.shape[1:], lambda e: (e, 0, 0))

    back_shape = jax.ShapeDtypeStruct(flat[0].shape, bf16)
    filled = (1 + peers) * pad
    outs = pl.pallas_call(
        functools.partial(expert_kernel, peers, parts, capacity, pad),
        grid=(experts,),
        out_shape=[jax.ShapeDtypeStruct((rows, width), f32)] + [back_shape] * len(flat),
        in_specs=[vm] * (parts + len(flat) + 2) + [per_expert(a) for a in (gate, up, down)],
        out_specs=[vm] * (1 + len(flat)),
        scratch_shapes=[
            pltpu.VMEM((experts, filled, width), bf16),
            pltpu.VMEM((1 + peers, experts * pad, width), bf16),
            pltpu.VMEM((experts * pad, rows), bf16),
            pltpu.VMEM((experts * pad, rows), bf16),
            pltpu.VMEM((experts * pad, flat[0].shape[0]), bf16),
        ],
        compiler_params=pltpu.CompilerParams(
            vmem_limit_bytes=48 * 2**20, dimension_semantics=("arbitrary",)
        ),
        cost_estimate=pl.CostEstimate(
            flops=6 * experts * filled * width * hidden,
            bytes_accessed=6 * experts * width * hidden,
            transcendentals=experts * filled * hidden,
        ),
        name="experts",
    )(*line, *flat, rank, share, gate, up, down)
    return outs[0], [outs[1 + j * parts : 1 + (j + 1) * parts] for j in range(peers)]


def shards(
    resid,
    pool_in,
    pool_weight,
    pool_scale,
    out_weight,
    norm_gain,
    route_ids,
    route_weight,
    expert_gate,
    expert_up,
    expert_down,
    shared_gate,
    shared_up,
    shared_down,
):
    n_sp, n_tp = lax.axis_size("sp"), lax.axis_size("tp")
    inner = n_sp // outer
    plane = lax.axis_index("sp") // inner
    lane = lax.axis_index("sp") % inner
    mine = lax.axis_index("tp")
    rows_here, top_count = route_ids.shape
    experts_here = expert_gate.shape[0]
    expert_total = experts_here * n_sp
    capacity = rows_here * top_count * 3 // (2 * expert_total)

    def along_outer(x, pairs):
        pairs = [(a * inner + i, b * inner + i) for a, b in pairs for i in range(inner)]
        return lax.ppermute(x, "sp", pairs)

    def along_inner(x, by):
        pairs = [
            (a * inner + i, a * inner + (i + by) % inner)
            for a in range(outer)
            for i in range(inner)
        ]
        return lax.ppermute(x, "sp", pairs)

    def along_tp(x, bits):
        return lax.ppermute(x, "tp", [(i, i ^ bits) for i in range(n_tp)])

    ups = [(0, 1), (1, 2), (2, 3)]
    downs = [(3, 2), (2, 1), (1, 0)]

    columns = out_weight.shape[1] // 2
    cross = [along_tp(out_weight[:, :columns], 2), along_tp(out_weight[:, columns:], 2)]
    weights = [
        [out_weight],
        [along_tp(out_weight, 1)],
        cross,
        [along_tp(cross[0], 1), along_tp(cross[1], 1)],
    ]
    resid_up = along_outer(resid, ups)
    resid_down = along_outer(resid, downs)

    ids = route_ids.T
    chosen = route_weight.T
    numbers = lax.iota(jnp.int32, expert_total)[:, None]
    member = jnp.zeros((expert_total, rows_here), jnp.bool_)
    share = jnp.zeros((expert_total, rows_here), f32)
    for k in range(top_count):
        hit = ids[k][None, :] == numbers
        member = member | hit
        share = share + jnp.where(hit, chosen[k][None, :], 0.0)
    order = lax.iota(jnp.int32, rows_here)
    ahead = (order[:, None] < order[None, :]).astype(bf16)
    seat = jnp.dot(member.astype(bf16), ahead, preferred_element_type=f32)
    seat = jnp.where(member, seat, -1.0)
    per_plane = inner * experts_here
    table = jnp.stack(
        [seat.reshape(outer, per_plane, rows_here), share.reshape(outer, per_plane, rows_here)],
        axis=1,
    )

    def table_for(by):
        return lax.dynamic_index_in_dim(table, lax.rem(plane + by, outer), axis=0, keepdims=False)

    tables = [table_for(0)]
    for by in range(1, outer):
        tables.append(along_outer(table_for(by), [(a, (a + by) % outer) for a in range(outer)]))
    low = plane <= 1
    slot_tables = [
        tables[0],
        jnp.where(low, tables[3], tables[1]),
        tables[2],
        jnp.where(low, tables[1], tables[3]),
    ]
    slots = range(4)
    peers = range(1, inner)

    def group_of(slot, by):
        start = lax.rem(lane + by, inner) * experts_here
        return lax.dynamic_slice_in_dim(slot_tables[slot], start, experts_here, axis=1)

    seats_out = experts_here * capacity
    line_no = lax.iota(jnp.int32, seats_out)
    spreader = (
        lax.div(line_no, capacity)[:, None] == lax.iota(jnp.int32, experts_here)[None, :]
    ).astype(bf16)
    seat_no = lax.rem(line_no, capacity).astype(f32)[:, None]
    send_pick = [[] for _ in slots]
    send_mix = [[] for _ in slots]
    for k in slots:
        for j in peers:
            t = group_of(k, j).astype(bf16)
            wide_rank = jnp.dot(spreader, t[0], preferred_element_type=f32)
            wide_share = jnp.dot(spreader, t[1], preferred_element_type=f32)
            hit = wide_rank == seat_no
            send_pick[k].append(hit.astype(bf16))
            send_mix[k].append(jnp.where(hit, wide_share, 0.0).astype(bf16))

    def exchange(slot, rows):
        got = []
        for j in peers:
            sent = jnp.dot(send_pick[slot][j - 1], rows, preferred_element_type=f32).astype(bf16)
            got.append(along_inner(sent, j))
        return got

    second_up = along_outer(resid_up, ups[1:])
    second_down = along_outer(resid_down, downs[1:])
    near_resid = jnp.where(low, resid_down, resid_up)
    spare_resid = jnp.where(
        plane == 1, resid_up, jnp.where(plane == 2, resid_down, jnp.zeros_like(resid))
    )
    other_resid = exchange(0, resid)
    other_near_resid = exchange(1, near_resid)

    pooled = pool_mix(pool_in, pool_weight, pool_scale)

    def pooled_for(bits):
        return lax.dynamic_slice_in_dim(pooled, (mine ^ bits) * rows_here, rows_here, axis=0)

    pieces = [pooled_for(0)] + [along_tp(pooled_for(b), b) for b in range(1, n_tp)]
    pooled = jnp.concatenate(pieces, axis=1)
    pooled_up = along_outer(pooled, ups)
    pooled_down = along_outer(pooled, downs)
    second_pooled = along_outer(pooled_up, ups[1:]) + along_outer(pooled_down, downs[1:])
    near_pooled = jnp.where(low, pooled_down, pooled_up)
    spare_pooled = jnp.where(
        plane == 1, pooled_up, jnp.where(plane == 2, pooled_down, jnp.zeros_like(pooled))
    )
    other_pooled = exchange(0, pooled)
    other_near_pooled = exchange(1, near_pooled)

    normed, *other_normed, middle = out_norm(
        [pooled, *other_pooled], [resid, *other_resid], norm_gain, weights, True
    )
    (second,) = out_norm(
        [second_pooled], [second_up + second_down], norm_gain, weights, False
    )
    near, spare, *other_near = out_norm(
        [near_pooled, spare_pooled, *other_near_pooled],
        [near_resid, spare_resid, *other_near_resid],
        norm_gain,
        weights,
        False,
    )

    far = []
    for h in range(2):
        half = second[:, h * columns : (h + 1) * columns]
        got_up = along_outer(half, ups[2:])
        got_down = along_outer(half, downs[2:])
        if far:
            got_up, got_down, _ = lax.optimization_barrier((got_up, got_down, far[0]))
        far.append(spare[:, h * columns : (h + 1) * columns] + got_up + got_down)

    lines = [[normed], [near], [second], far]
    arrived = [
        [[o] for o in other_normed],
        [[o] for o in other_near],
        [[o] for o in exchange(2, second)],
        [list(pair) for pair in zip(exchange(3, far[0]), exchange(3, far[1]))],
    ]
    owns, backs = [], []
    for k in slots:
        own_table = group_of(k, 0)
        own, back = run_experts(
            lines[k],
            arrived[k],
            own_table[0],
            own_table[1],
            expert_gate,
            expert_up,
            expert_down,
            capacity,
        )
        owns.append(own)
        backs.append(back)

    def partial_sum(k):
        halves = []
        whole = None
        for h in range(2):
            if len(backs[k][0]) == 2:
                parts = [along_inner(backs[k][j - 1][h], -j) for j in peers]
            else:
                if whole is None:
                    whole = [along_inner(backs[k][j - 1][0], -j) for j in peers]
                parts = whole
            halves.append(combine(owns[k], send_mix[k], parts, h))
        return halves

    sums = [partial_sum(k) for k in slots]

    shared_hidden = (
        jax.nn.silu(jnp.dot(normed, shared_gate, preferred_element_type=f32))
        * jnp.dot(normed, shared_up, preferred_element_type=f32)
    ).astype(bf16)
    base = lax.optimization_barrier(
        middle.astype(f32)
        + jnp.dot(shared_hidden, shared_down, preferred_element_type=f32)
    )

    last_up, last_down = [], []
    for h in range(2):
        got_up = along_outer(sums[3][h], ups[:1])
        got_down = along_outer(sums[3][h], downs[:1])
        mid = sums[2][h] + got_up + got_down
        got_up = along_outer(mid, ups[:2])
        got_down = along_outer(mid, downs[:2])
        near_up = jnp.where(plane == 2, sums[3][h], sums[1][h]) + got_up
        near_down = jnp.where(plane == 1, sums[3][h], sums[1][h]) + got_down
        last_up.append(along_outer(near_up, ups))
        last_down.append(along_outer(near_down, downs))
    return finish(base, *sums[0], *last_up, *last_down)


def solution(mesh):
    return jax.shard_map(
        shards,
        mesh=mesh,
        in_specs=(
            P(("sp", "tp"), None),
            P("sp", "tp"),
            P("tp", None, None),
            P("tp"),
            P("tp", None),
            P(),
            P(("sp", "tp"), None),
            P(("sp", "tp"), None),
            P("sp", None, None),
            P("sp", None, None),
            P("sp", None, None),
            P(),
            P(),
            P(),
        ),
        out_specs=P(("sp", "tp"), None),
        check_vma=False,
    )
```

```python
import functools

import jax
import jax.numpy as jnp
from jax import lax
from jax.experimental import pallas as pl
from jax.experimental.pallas import tpu as pltpu
from jax.sharding import PartitionSpec as P


reach_rows = 8
norm_eps = 1e-06
outer = 4


f32 = jnp.float32
bf16 = jnp.bfloat16


def with_halo(cells, axis, width):
    count = lax.axis_size(axis)
    ends = count - 1
    head = cells[:width]
    tail = cells[cells.shape[0] - width :]
    return jnp.concatenate(
        [
            lax.ppermute(tail, axis, [(i, i + 1) for i in range(ends)]),
            cells,
            lax.ppermute(head, axis, [(i + 1, i) for i in range(ends)]),
        ],
        axis=0,
    )


def window_means(padded, length, offset, whole_len):
    positions = offset + lax.iota(jnp.int32, length)
    running = jnp.zeros((length,) + padded.shape[1:], f32)
    averages = []
    covered = 0
    for section_num in range(4):
        half_span = 2**section_num
        for row_shift in list(range(-half_span, -covered)) + list(range(covered, half_span)):
            running = running + padded[reach_rows + row_shift : reach_rows + row_shift + length]
        covered = half_span
        upper_end = jnp.minimum(positions + half_span, whole_len)
        lower_end = jnp.maximum(positions - half_span, 0)
        row_count = (upper_end - lower_end).astype(f32)
        averages.append(running / row_count[:, None, None])
    return averages


def pool_mix(pool_in, pool_weight, pool_scale):
    tok_local = pool_in.shape[0]
    local_groups, group_width = pool_weight.shape[:2]
    padded = with_halo(pool_in, "sp", reach_rows).astype(f32)
    padded = padded.reshape(tok_local + 2 * reach_rows, local_groups, group_width)
    averages = window_means(
        padded, tok_local, lax.axis_index("sp") * tok_local, tok_local * lax.axis_size("sp")
    )
    center = padded[reach_rows : reach_rows + tok_local]
    group_ids = lax.axis_index("tp") * local_groups + lax.iota(jnp.int32, local_groups)
    chosen = averages[0]
    for section_num in range(1, 4):
        chosen = jnp.where((group_ids == section_num)[None, :, None], averages[section_num], chosen)
    spread = (chosen - center).astype(bf16)
    mixed_rows = jnp.einsum("tgc,gce->tge", spread, pool_weight, preferred_element_type=f32)
    return (mixed_rows.reshape(tok_local, -1) * pool_scale[None, :]).astype(bf16)


def out_norm_kernel(blocks, keep, halved, *refs):
    pools, resids = refs[:blocks], refs[blocks : 2 * blocks]
    refs = refs[2 * blocks :]
    gain, refs = refs[0], refs[1:]
    weights = []
    for parts in halved:
        weights.append(refs[:parts])
        refs = refs[parts:]
    outs = refs
    width = gain.shape[1]
    depth = weights[0][0].shape[0]
    step = 1024
    steps = width // step

    def part(n):
        return pl.ds(pl.multiple_of(n * step, step), step)

    for i in range(blocks):
        pool, resid = pools[i], resids[i]
        normed = outs[i]
        middle = outs[blocks] if keep and i == 0 else normed

        def project(half, n, total):
            at = part(n + half * (steps // 2))
            acc = resid[:, at].astype(f32)
            for j, weight in enumerate(weights):
                rows = weight[half][:, part(n)] if len(weight) == 2 else weight[0][:, at]
                acc = acc + jnp.dot(
                    pool[:, j * depth : (j + 1) * depth], rows, preferred_element_type=f32
                )
            mid = acc.astype(bf16)
            middle[:, at] = mid
            mid = mid.astype(f32)
            return total + jnp.sum(mid * mid, axis=1, keepdims=True)

        total = jnp.zeros((resid.shape[0], 1), f32)
        for half in range(2):
            total = lax.fori_loop(0, steps // 2, functools.partial(project, half), total)
        scale = lax.rsqrt(total * (1.0 / width) + norm_eps)

        def finish(n, carry):
            at = part(n)
            normed[:, at] = (middle[:, at].astype(f32) * scale * gain[:, at]).astype(bf16)
            return carry

        lax.fori_loop(0, steps, finish, 0)


def out_norm(pools, resids, gain, weights, keep):
    blocks = len(pools)
    vm = pl.BlockSpec(memory_space=pltpu.VMEM)
    shapes = [jax.ShapeDtypeStruct(r.shape, bf16) for r in resids]
    shapes += [shapes[0]] * (1 if keep else 0)
    rows = sum(r.shape[0] for r in resids)
    flat = [w for group in weights for w in group]
    return pl.pallas_call(
        functools.partial(out_norm_kernel, blocks, keep, [len(g) for g in weights]),
        out_shape=shapes,
        in_specs=[vm] * (2 * blocks + 1 + len(flat)),
        out_specs=[vm] * len(shapes),
        compiler_params=pltpu.CompilerParams(vmem_limit_bytes=36 * 2**20),
        cost_estimate=pl.CostEstimate(
            flops=2 * rows * pools[0].shape[1] * gain.shape[0],
            bytes_accessed=4 * rows * gain.shape[0],
            transcendentals=rows,
        ),
        name="out_norm",
    )(*pools, *resids, gain.reshape(1, -1), *flat)


def combine_kernel(count, own, *refs):
    mixes, parts, out = refs[:count], refs[count : 2 * count], refs[2 * count]
    total = own[...]
    for mix, part in zip(mixes, parts):
        total = total + lax.dot_general(
            mix[...], part[...], (((0,), (0,)), ((), ())), preferred_element_type=f32
        )
    out[...] = total.astype(bf16)


def combine(own, mixes, parts, half):
    count = len(parts)
    rows, width = own.shape
    step = width // 4
    skip = 2 * half
    cut_parts = parts[0].shape[1] == width
    whole = [pl.BlockSpec(m.shape, lambda n: (0, 0)) for m in mixes]
    cut = [
        pl.BlockSpec((p.shape[0], step), lambda n: (0, n + (skip if cut_parts else 0)))
        for p in parts
    ]
    return pl.pallas_call(
        functools.partial(combine_kernel, count),
        grid=(2,),
        out_shape=jax.ShapeDtypeStruct((rows, width // 2), bf16),
        in_specs=[pl.BlockSpec((rows, step), lambda n: (0, n + skip))] + whole + cut,
        out_specs=pl.BlockSpec((rows, step), lambda n: (0, n)),
        compiler_params=pltpu.CompilerParams(vmem_limit_bytes=24 * 2**20),
        cost_estimate=pl.CostEstimate(
            flops=rows * width * sum(p.shape[0] for p in parts),
            bytes_accessed=4 * rows * width,
            transcendentals=0,
        ),
        name="combine",
    )(own, *mixes, *parts)


def finish_kernel(base, own_a, own_b, up_a, up_b, down_a, down_b, out):
    span = own_a.shape[1]
    for h, group in enumerate(((own_a, up_a, down_a), (own_b, up_b, down_b))):
        at = slice(h * span, (h + 1) * span)
        total = base[:, at]
        for part in group:
            total = total + part[...].astype(f32)
        out[:, at] = total.astype(bf16)


def finish(base, *parts):
    vm = pl.BlockSpec(memory_space=pltpu.VMEM)
    return pl.pallas_call(
        finish_kernel,
        out_shape=jax.ShapeDtypeStruct(base.shape, bf16),
        in_specs=[vm] * (1 + len(parts)),
        out_specs=vm,
        compiler_params=pltpu.CompilerParams(vmem_limit_bytes=20 * 2**20),
        name="finish",
    )(base, *parts)


def expert_kernel(peers, shape, capacity, pad, *refs):
    slots = len(shape)
    lines, others = [], []
    for parts in shape:
        lines.append(refs[:parts])
        refs = refs[parts:]
    for parts in shape:
        others.append([refs[j * parts : (j + 1) * parts] for j in range(peers)])
        refs = refs[peers * parts :]
    ranks, shares, refs = refs[:slots], refs[slots : 2 * slots], refs[2 * slots :]
    gate, up, down = refs[:3]
    owns, refs = refs[3 : 3 + slots], refs[3 + slots :]
    backs = []
    for parts in shape:
        backs.append([refs[j * parts : (j + 1) * parts] for j in range(peers)])
        refs = refs[peers * parts :]
    packed, made, pick, mixing, shift = refs
    expert = pl.program_id(0)
    count = pl.num_programs(0)
    experts = ranks[0].shape[0]
    rows = lines[0][0].shape[0]
    other_rows = others[0][0][0].shape[0]
    step = 1024
    group = (1 + peers) * pad
    filled, width = packed.shape[1:]
    wide = gate.shape[2]

    def columns(n, skip=0):
        return pl.ds(pl.multiple_of(skip + n * step, step), step)

    @pl.when(expert == 0)
    def _():
        seat = lax.broadcasted_iota(jnp.int32, (pad, rows), 0).astype(f32)
        seat = jnp.where(seat < capacity, seat, -2.0)
        row = lax.broadcasted_iota(jnp.int32, (pad, other_rows), 0)
        col = lax.broadcasted_iota(jnp.int32, (pad, other_rows), 1)
        for e in range(experts):
            here = slice(e * pad, (e + 1) * pad)
            for k in range(slots):
                hit = ranks[k][e : e + 1, :] == seat
                pick[k, here, :] = hit.astype(f32).astype(bf16)
                mixing[k, here, :] = jnp.where(hit, shares[k][e : e + 1, :], 0.0).astype(bf16)
            shift[here, :] = (
                ((col == e * capacity + row) & (row < capacity)).astype(f32).astype(bf16)
            )
        for k, parts in enumerate(shape):
            span = width // parts
            for h in range(parts):

                def gather(n, carry):
                    for i in range(1 + peers):
                        source = lines[k] if i == 0 else others[k][i - 1]
                        chooser = pick[k] if i == 0 else shift[...]
                        moved = jnp.dot(
                            chooser, source[h][:, columns(n)], preferred_element_type=f32
                        ).astype(bf16)
                        at = k * group + i * pad
                        for e in range(experts):
                            packed[e, at : at + pad, columns(n, h * span)] = moved[
                                e * pad : (e + 1) * pad
                            ]
                    return carry

                lax.fori_loop(0, span // step, gather, 0)

    even = wide // 256 * 256
    shared_tile = wide - even == 128 and even > 0

    def project(n, carry):
        at = columns(n)
        tokens = packed[expert, :, at]
        if shared_tile:
            mixed = jnp.concatenate([gate[0, at, even:], up[0, at, :128]], axis=1)
            blocks = (gate[0, at, :even], mixed, up[0, at, 128:])
        else:
            blocks = (gate[0, at, :], up[0, at, :])
        return tuple(
            c + jnp.dot(tokens, w, preferred_element_type=f32) for c, w in zip(carry, blocks)
        )

    spans = (even, 256, even) if shared_tile else (wide, wide)
    sums = lax.fori_loop(
        0, width // step, project, tuple(jnp.zeros((filled, n), f32) for n in spans)
    )
    if shared_tile:
        gated = jnp.concatenate([sums[0], sums[1][:, :128]], axis=1)
        lifted = jnp.concatenate([sums[1][:, 128:], sums[2]], axis=1)
    else:
        gated, lifted = sums
    hidden = (gated * (1.0 / (1.0 + jnp.exp(-gated))) * lifted).astype(bf16)

    def lower(n, carry):
        at = columns(n)
        result = jnp.dot(hidden, down[0, :, at], preferred_element_type=f32).astype(bf16)
        for i in range(slots * (1 + peers)):
            made[i, pl.ds(pl.multiple_of(expert * pad, pad), pad), at] = result[
                i * pad : (i + 1) * pad
            ]
        return carry

    lax.fori_loop(0, width // step, lower, 0)

    @pl.when(expert == count - 1)
    def _():
        rows_in = (((0,), (0,)), ((), ()))
        for k, parts in enumerate(shape):
            span = width // parts
            for h in range(parts):

                def spread(n, carry):
                    come = columns(n, h * span)
                    at = k * (1 + peers)
                    owns[k][:, come] = lax.dot_general(
                        mixing[k], made[at, :, come], rows_in, preferred_element_type=f32
                    )
                    for j in range(peers):
                        backs[k][j][h][:, columns(n)] = lax.dot_general(
                            shift[...],
                            made[at + 1 + j, :, come],
                            rows_in,
                            preferred_element_type=f32,
                        ).astype(bf16)
                    return carry

                lax.fori_loop(0, span // step, spread, 0)


def run_experts(lines, others, ranks, shares, gate, up, down, capacity):
    slots = len(lines)
    peers = len(others[0])
    shape = tuple(len(line) for line in lines)
    experts, width, hidden = gate.shape
    pad = -(-capacity // 16) * 16
    rows = lines[0][0].shape[0]
    vm = pl.BlockSpec(memory_space=pltpu.VMEM)
    flat_lines = [h for line in lines for h in line]
    flat = [h for slot in others for pair in slot for h in pair]

    def per_expert(a):
        return pl.BlockSpec((1,) + a.shape[1:], lambda e: (e, 0, 0))

    filled = slots * (1 + peers) * pad
    outs = pl.pallas_call(
        functools.partial(expert_kernel, peers, shape, capacity, pad),
        grid=(experts,),
        out_shape=[jax.ShapeDtypeStruct((rows, width), f32)] * slots
        + [jax.ShapeDtypeStruct(a.shape, bf16) for a in flat],
        in_specs=[vm] * (len(flat_lines) + len(flat) + 2 * slots)
        + [per_expert(a) for a in (gate, up, down)],
        out_specs=[vm] * (slots + len(flat)),
        scratch_shapes=[
            pltpu.VMEM((experts, filled, width), bf16),
            pltpu.VMEM((slots * (1 + peers), experts * pad, width), bf16),
            pltpu.VMEM((slots, experts * pad, rows), bf16),
            pltpu.VMEM((slots, experts * pad, rows), bf16),
            pltpu.VMEM((experts * pad, flat[0].shape[0]), bf16),
        ],
        compiler_params=pltpu.CompilerParams(
            vmem_limit_bytes=56 * 2**20, dimension_semantics=("arbitrary",)
        ),
        cost_estimate=pl.CostEstimate(
            flops=6 * experts * filled * width * hidden,
            bytes_accessed=6 * experts * width * hidden,
            transcendentals=experts * filled * hidden,
        ),
        name="experts",
    )(*flat_lines, *flat, *ranks, *shares, gate, up, down)
    owns, outs = list(outs[:slots]), outs[slots:]
    backs = []
    for parts in shape:
        backs.append([outs[j * parts : (j + 1) * parts] for j in range(peers)])
        outs = outs[peers * parts :]
    return owns, backs


def shards(
    resid,
    pool_in,
    pool_weight,
    pool_scale,
    out_weight,
    norm_gain,
    route_ids,
    route_weight,
    expert_gate,
    expert_up,
    expert_down,
    shared_gate,
    shared_up,
    shared_down,
):
    n_sp, n_tp = lax.axis_size("sp"), lax.axis_size("tp")
    inner = n_sp // outer
    plane = lax.axis_index("sp") // inner
    lane = lax.axis_index("sp") % inner
    mine = lax.axis_index("tp")
    rows_here, top_count = route_ids.shape
    experts_here = expert_gate.shape[0]
    expert_total = experts_here * n_sp
    capacity = rows_here * top_count * 3 // (2 * expert_total)

    def along_outer(x, pairs):
        pairs = [(a * inner + i, b * inner + i) for a, b in pairs for i in range(inner)]
        return lax.ppermute(x, "sp", pairs)

    def along_inner(x, by):
        pairs = [
            (a * inner + i, a * inner + (i + by) % inner)
            for a in range(outer)
            for i in range(inner)
        ]
        return lax.ppermute(x, "sp", pairs)

    def along_tp(x, bits):
        return lax.ppermute(x, "tp", [(i, i ^ bits) for i in range(n_tp)])

    ups = [(0, 1), (1, 2), (2, 3)]
    downs = [(3, 2), (2, 1), (1, 0)]

    columns = out_weight.shape[1] // 2
    cross = [along_tp(out_weight[:, :columns], 2), along_tp(out_weight[:, columns:], 2)]
    weights = [
        [out_weight],
        [along_tp(out_weight, 1)],
        cross,
        [along_tp(cross[0], 1), along_tp(cross[1], 1)],
    ]
    resid_up = along_outer(resid, ups)
    resid_down = along_outer(resid, downs)

    ids = route_ids.T
    chosen = route_weight.T
    numbers = lax.iota(jnp.int32, expert_total)[:, None]
    member = jnp.zeros((expert_total, rows_here), jnp.bool_)
    share = jnp.zeros((expert_total, rows_here), f32)
    for k in range(top_count):
        hit = ids[k][None, :] == numbers
        member = member | hit
        share = share + jnp.where(hit, chosen[k][None, :], 0.0)
    order = lax.iota(jnp.int32, rows_here)
    ahead = (order[:, None] < order[None, :]).astype(bf16)
    seat = jnp.dot(member.astype(bf16), ahead, preferred_element_type=f32)
    seat = jnp.where(member, seat, -1.0)
    per_plane = inner * experts_here
    table = jnp.stack(
        [seat.reshape(outer, per_plane, rows_here), share.reshape(outer, per_plane, rows_here)],
        axis=1,
    )

    def table_for(by):
        return lax.dynamic_index_in_dim(table, lax.rem(plane + by, outer), axis=0, keepdims=False)

    tables = [table_for(0)]
    for by in range(1, outer):
        tables.append(along_outer(table_for(by), [(a, (a + by) % outer) for a in range(outer)]))
    low = plane <= 1
    slot_tables = [
        tables[0],
        jnp.where(low, tables[3], tables[1]),
        tables[2],
        jnp.where(low, tables[1], tables[3]),
    ]
    slots = range(4)
    peers = range(1, inner)

    def group_of(slot, by):
        start = lax.rem(lane + by, inner) * experts_here
        return lax.dynamic_slice_in_dim(slot_tables[slot], start, experts_here, axis=1)

    seats_out = experts_here * capacity
    line_no = lax.iota(jnp.int32, seats_out)
    spreader = (
        lax.div(line_no, capacity)[:, None] == lax.iota(jnp.int32, experts_here)[None, :]
    ).astype(bf16)
    seat_no = lax.rem(line_no, capacity).astype(f32)[:, None]
    send_pick = [[] for _ in slots]
    send_mix = [[] for _ in slots]
    for k in slots:
        for j in peers:
            t = group_of(k, j).astype(bf16)
            wide_rank = jnp.dot(spreader, t[0], preferred_element_type=f32)
            wide_share = jnp.dot(spreader, t[1], preferred_element_type=f32)
            hit = wide_rank == seat_no
            send_pick[k].append(hit.astype(bf16))
            send_mix[k].append(jnp.where(hit, wide_share, 0.0).astype(bf16))

    def exchange(slot, rows):
        got = []
        for j in peers:
            sent = jnp.dot(send_pick[slot][j - 1], rows, preferred_element_type=f32).astype(bf16)
            got.append(along_inner(sent, j))
        return got

    second_up = along_outer(resid_up, ups[1:])
    second_down = along_outer(resid_down, downs[1:])
    near_resid = jnp.where(low, resid_down, resid_up)
    spare_resid = jnp.where(
        plane == 1, resid_up, jnp.where(plane == 2, resid_down, jnp.zeros_like(resid))
    )
    other_resid = exchange(0, resid)
    other_near_resid = exchange(1, near_resid)

    pooled = pool_mix(pool_in, pool_weight, pool_scale)

    def pooled_for(bits):
        return lax.dynamic_slice_in_dim(pooled, (mine ^ bits) * rows_here, rows_here, axis=0)

    pieces = [pooled_for(0)] + [along_tp(pooled_for(b), b) for b in range(1, n_tp)]
    pooled = jnp.concatenate(pieces, axis=1)
    pooled_up = along_outer(pooled, ups)
    pooled_down = along_outer(pooled, downs)
    second_pooled = along_outer(pooled_up, ups[1:]) + along_outer(pooled_down, downs[1:])
    near_pooled = jnp.where(low, pooled_down, pooled_up)
    spare_pooled = jnp.where(
        plane == 1, pooled_up, jnp.where(plane == 2, pooled_down, jnp.zeros_like(pooled))
    )
    other_pooled = exchange(0, pooled)
    other_near_pooled = exchange(1, near_pooled)

    normed, *other_normed, middle = out_norm(
        [pooled, *other_pooled], [resid, *other_resid], norm_gain, weights, True
    )
    (second,) = out_norm(
        [second_pooled], [second_up + second_down], norm_gain, weights, False
    )
    near, spare, *other_near = out_norm(
        [near_pooled, spare_pooled, *other_near_pooled],
        [near_resid, spare_resid, *other_near_resid],
        norm_gain,
        weights,
        False,
    )

    far = []
    for h in range(2):
        half = second[:, h * columns : (h + 1) * columns]
        got_up = along_outer(half, ups[2:])
        got_down = along_outer(half, downs[2:])
        if far:
            got_up, got_down, _ = lax.optimization_barrier((got_up, got_down, far[0]))
        far.append(spare[:, h * columns : (h + 1) * columns] + got_up + got_down)

    lines = [[normed], [near], [second], far]
    arrived = [
        [[o] for o in other_normed],
        [[o] for o in other_near],
        [[o] for o in exchange(2, second)],
        [list(pair) for pair in zip(exchange(3, far[0]), exchange(3, far[1]))],
    ]
    owns, backs = [], []
    for batch in ((0, 1), (2, 3)):
        own_tables = [group_of(k, 0) for k in batch]
        got_own, got_back = run_experts(
            [lines[k] for k in batch],
            [arrived[k] for k in batch],
            [t[0] for t in own_tables],
            [t[1] for t in own_tables],
            expert_gate,
            expert_up,
            expert_down,
            capacity,
        )
        owns += got_own
        backs += got_back

    def partial_sum(k):
        halves = []
        whole = None
        for h in range(2):
            if len(backs[k][0]) == 2:
                parts = [along_inner(backs[k][j - 1][h], -j) for j in peers]
            else:
                if whole is None:
                    whole = [along_inner(backs[k][j - 1][0], -j) for j in peers]
                parts = whole
            halves.append(combine(owns[k], send_mix[k], parts, h))
        return halves

    sums = [partial_sum(k) for k in slots]

    shared_hidden = (
        jax.nn.silu(jnp.dot(normed, shared_gate, preferred_element_type=f32))
        * jnp.dot(normed, shared_up, preferred_element_type=f32)
    ).astype(bf16)
    base = lax.optimization_barrier(
        middle.astype(f32)
        + jnp.dot(shared_hidden, shared_down, preferred_element_type=f32)
    )

    last_up, last_down = [], []
    for h in range(2):
        got_up = along_outer(sums[3][h], ups[:1])
        got_down = along_outer(sums[3][h], downs[:1])
        mid = sums[2][h] + got_up + got_down
        got_up = along_outer(mid, ups[:2])
        got_down = along_outer(mid, downs[:2])
        near_up = jnp.where(plane == 2, sums[3][h], sums[1][h]) + got_up
        near_down = jnp.where(plane == 1, sums[3][h], sums[1][h]) + got_down
        last_up.append(along_outer(near_up, ups))
        last_down.append(along_outer(near_down, downs))
    return finish(base, *sums[0], *last_up, *last_down)


def solution(mesh):
    return jax.shard_map(
        shards,
        mesh=mesh,
        in_specs=(
            P(("sp", "tp"), None),
            P("sp", "tp"),
            P("tp", None, None),
            P("tp"),
            P("tp", None),
            P(),
            P(("sp", "tp"), None),
            P(("sp", "tp"), None),
            P("sp", None, None),
            P("sp", None, None),
            P("sp", None, None),
            P(),
            P(),
            P(),
        ),
        out_specs=P(("sp", "tp"), None),
        check_vma=False,
    )
```
